32 devices in a mesh: sp: 16 (over z, y, x), tp: 2 (over core).
Axes of the slice: x: 2, y: 2, z: 4, core: 2. Of those that a mesh axis runs over, the one named last changes fastest.
Arguments:
- tokens_in: bfloat16 [4096, 2048], P('sp', 'tp'), may hold values from -720 to 720
- norm_gain: float32 [2048], replicated, may hold values from 0.1 to 1.9
- recept_weight: bfloat16 [2048, 2048], P('sp', 'tp'), may hold values from -0.125 to 0.125
- key_weight: bfloat16 [2048, 2048], P('sp', 'tp'), may hold values from -0.125 to 0.125
- value_weight: bfloat16 [2048, 2048], P('sp', 'tp'), may hold values from -0.125 to 0.125
- decay_weight: bfloat16 [2048, 2048], P('sp', 'tp'), may hold values from -0.0625 to 0.0625
- outer_weight: bfloat16 [2048, 2048], P('sp', 'tp'), may hold values from -0.125 to 0.125
- inner_weight: bfloat16 [2048, 2048], P('sp', 'tp'), may hold values from -0.125 to 0.125
- conv_weight: bfloat16 [2048, 2048], P('sp', 'tp'), may hold values from -0.125 to 0.125
- conv_taps: bfloat16 [3, 2048], P(None, 'tp'), may hold values from -3.5 to 3.5
- decay_base: float32 [2048], P('tp'), may hold values from -12 to -2
- decay_shift: float32 [4096, 2048], P('sp', 'tp'), may hold values from -1 to 12
- rate_logit: float32 [2048], P('tp'), may hold values from -12 to 2
- head_gain: float32 [2048], P('tp'), may hold values from 0.1 to 1.9
- readout_projector: bfloat16 [4096, 2048], P('sp', 'tp'), may hold values from -0.09375 to 0.09375
Outputs:
- mixed: bfloat16 [4096, 2048], P('sp', 'tp')
The draws below stay inside these ranges and needn't reach their ends.
All inputs are finite; a program needn't handle non-finite values.
Results may differ from the reference program's by a relative error of at most 0.015.
Values may be sent and summed in bfloat16 or wider, within the bound.
A program may use at most 128 MiB of HBM per device.

```python
import math
import jax
import jax.numpy as jnp
from jax import lax

D = 2048
MIX_WIDTH = 2048
HEAD_SIZE = 64
TAPS = 3
TOK_DEV = 256
HEADS = 32
STREAM_LENGTH = 4096


def decay_law(key):
    first, latter_operand, third, fourth = jax.random.split(jax.random.fold_in(key, 7), 4)
    share = 0.5
    slow = jax.random.bernoulli(first, share, (MIX_WIDTH // HEAD_SIZE,))
    slow = jnp.repeat(slow, HEAD_SIZE)
    log_length = math.log(STREAM_LENGTH)
    base = jnp.where(slow, 0.5 - log_length, -3.2) + jax.random.uniform(latter_operand, (MIX_WIDTH,), jnp.float32, -0.5, 0.5)
    gradual_forgetting = math.log(HEAD_SIZE / STREAM_LENGTH) + jax.random.uniform(third, (MIX_WIDTH,), jnp.float32, -0.7, 0.3)
    fast_rate = jax.random.uniform(fourth, (MIX_WIDTH,), jnp.float32, -2.0, 2.0)
    return (base, jnp.where(slow, gradual_forgetting, fast_rate))


def draw_decay_base(key, part):
    return decay_law(key)[0].astype(jnp.float32)


def draw_rate_logit(key, part):
    return decay_law(key)[1].astype(jnp.float32)


def draw_decay_shift(key, part):
    first, latter_operand = jax.random.split(jax.random.fold_in(key, 5), 2)
    forgetting_factor_grid = jax.random.uniform(first, (STREAM_LENGTH // TOK_DEV, MIX_WIDTH), jnp.float32, -0.7, 0.7)
    forgetting_factor_grid = jnp.repeat(forgetting_factor_grid, TOK_DEV, axis=0)
    drawn_indices = jax.random.randint(latter_operand, (4,), 0, STREAM_LENGTH)
    entry_cluster_extent = jnp.any(jnp.arange(STREAM_LENGTH)[:, None] == drawn_indices[None, :], axis=1)
    return (forgetting_factor_grid + jnp.where(entry_cluster_extent, math.log(STREAM_LENGTH), 0.0)[:, None]).astype(jnp.float32)


def draw_tokens_in(key, part):
    first, latter_operand, third = jax.random.split(jax.random.fold_in(key, 3), 3)
    row_scale = 10.0 ** jax.random.uniform(first, (STREAM_LENGTH, 1), jnp.float32)
    col_scale = 3.0 ** (jnp.arange(D, dtype=jnp.float32) / D) * 10.0 ** (0.75 * jax.random.uniform(latter_operand, (D,), jnp.float32))
    base = jnp.clip(jax.random.normal(third, (STREAM_LENGTH, D), jnp.float32), -4.0, 4.0)
    return (base * row_scale * col_scale).astype(jnp.bfloat16)


def block_levels(key, extent, cuts, smallest, high):
    loudness = 1.0
    for position, shards_of in cuts:
        heights = jax.random.uniform(jax.random.fold_in(jax.random.fold_in(key, 6), position), (shards_of,), jnp.float32, smallest / len(cuts), high / len(cuts))
        loudness = loudness * jnp.repeat(jnp.exp(heights), extent[position] // shards_of).reshape((-1,) + (1,) * (len(extent) - 1 - position))
    return loudness


def bell_draw(own_key, extent, deviation, limit, shards=(), kind=jnp.bfloat16):
    loudness = block_levels(own_key, extent, shards, -0.22, 0.18) if shards else 1.0
    drawn = jax.random.normal(own_key, extent, jnp.float32) * deviation * loudness
    return jnp.minimum(jnp.maximum(drawn, -limit), limit).astype(kind)


def setup_inputs(seed: int = 0) -> dict:
    seeds = jax.random.split(jax.random.key(seed), 16)
    return {
        "tokens_in": draw_tokens_in(jax.random.fold_in(seeds[15], 71), 0),
        "norm_gain": jnp.clip(1.0 + 0.18 * jax.random.normal(seeds[1], (D,), jnp.float32), 0.1, 1.9),
        "recept_weight": bell_draw(seeds[2], (D, MIX_WIDTH), D ** -0.5, 0.125, ((0, 16), (1, 2))),
        "key_weight": bell_draw(seeds[3], (D, MIX_WIDTH), D ** -0.5, 0.125, ((0, 16), (1, 2))),
        "value_weight": bell_draw(seeds[4], (D, MIX_WIDTH), D ** -0.5, 0.125, ((0, 16), (1, 2))),
        "decay_weight": bell_draw(seeds[5], (D, MIX_WIDTH), (4 * D) ** -0.5, 0.0625, ((0, 16), (1, 2))),
        "outer_weight": bell_draw(seeds[6], (D, MIX_WIDTH), D ** -0.5, 0.125, ((0, 16), (1, 2))),
        "inner_weight": bell_draw(seeds[7], (D, MIX_WIDTH), D ** -0.5, 0.125, ((0, 16), (1, 2))),
        "conv_weight": bell_draw(seeds[8], (D, MIX_WIDTH), D ** -0.5, 0.125, ((0, 16), (1, 2))),
        "conv_taps": bell_draw(seeds[9], (TAPS, MIX_WIDTH), TAPS ** -0.5, 3.5, ((1, 2),)),
        "decay_base": draw_decay_base(jax.random.fold_in(seeds[15], 71), 0),
        "decay_shift": draw_decay_shift(jax.random.fold_in(seeds[15], 71), 0),
        "rate_logit": draw_rate_logit(jax.random.fold_in(seeds[15], 71), 0),
        "head_gain": jnp.clip(1.0 + 0.18 * jax.random.normal(seeds[13], (MIX_WIDTH,), jnp.float32), 0.1, 1.9),
        "readout_projector": bell_draw(seeds[14], (2 * MIX_WIDTH, D), (2 * MIX_WIDTH) ** -0.5, 0.09375, ((0, 16), (1, 2))),
    }


norm_eps = 1e-05
group_eps = 0.00064
unit_eps = 1e-06

def layer_input(tokens_in, norm_gain):
    wide = tokens_in.astype(jnp.float32)
    center = lax.optimization_barrier(jnp.mean(wide, axis=-1, keepdims=True))
    variance = lax.optimization_barrier(jnp.mean(jnp.square(wide - center), axis=-1, keepdims=True))
    return ((wide - center) * lax.rsqrt(variance + norm_eps) * norm_gain).astype(jnp.bfloat16)

def project(normalized_rows, weight):
    return jnp.dot(normalized_rows, weight, preferred_element_type=jnp.float32).astype(jnp.bfloat16)

def state_steps(recept, keys, values, log_decay, rate):
    highest = lax.Precision.HIGHEST
    unit = keys * lax.rsqrt(lax.optimization_barrier(jnp.sum(keys * keys, axis=-1, keepdims=True)) + unit_eps)
    scaled = unit * rate

    def advance(state, inputs):
        query_now, key_now, value_now, decay_now, unit_now, scaled_now = inputs
        remove = jnp.einsum('hvk,hk->hv', state, unit_now, precision=highest)
        state = state * jnp.exp(decay_now)[:, None, :] - remove[:, :, None] * scaled_now[:, None, :] + value_now[:, :, None] * key_now[:, None, :]
        return (state, jnp.einsum('hvk,hk->hv', state, query_now, precision=highest))
    start = jnp.zeros((keys.shape[1], keys.shape[2], keys.shape[2]), jnp.float32)
    final, reads = lax.scan(advance, start, (recept, keys, values, log_decay, unit, scaled))
    return reads

def reference(tokens_in, norm_gain, recept_weight, key_weight, value_weight, decay_weight, outer_weight, inner_weight, conv_weight, conv_taps, decay_base, decay_shift, rate_logit, head_gain, readout_projector):
    normalized_rows = layer_input(tokens_in, norm_gain)
    recept = project(normalized_rows, recept_weight)
    keys = project(normalized_rows, key_weight)
    values = project(normalized_rows, value_weight)
    decay_proj = project(normalized_rows, decay_weight)
    outer = project(normalized_rows, outer_weight)
    inner = project(normalized_rows, inner_weight)
    conv_in = project(normalized_rows, conv_weight)
    gated = (inner.astype(jnp.float32) * conv_in.astype(jnp.float32)).astype(jnp.bfloat16)
    padded = jnp.concatenate([jnp.zeros((2, MIX_WIDTH), jnp.bfloat16), gated], axis=0).astype(jnp.float32)
    taps = conv_taps.astype(jnp.float32)
    conv_sum = taps[0] * padded[:-2] + taps[1] * padded[1:-1] + taps[2] * padded[2:]
    conv_branch = (outer.astype(jnp.float32) * conv_sum).astype(jnp.bfloat16)
    pre = decay_base + decay_proj.astype(jnp.float32) + decay_shift
    log_decay = -jnp.exp(-jax.nn.softplus(-pre) - 0.5)
    rate = jax.nn.sigmoid(rate_logit).reshape(HEADS, HEAD_SIZE)

    def heads(array):
        return array.astype(jnp.float32).reshape(STREAM_LENGTH, HEADS, HEAD_SIZE)
    reads = state_steps(heads(recept), heads(keys), heads(values), heads(log_decay), rate)
    center = lax.optimization_barrier(jnp.mean(reads, axis=-1, keepdims=True))
    variance = lax.optimization_barrier(jnp.mean(jnp.square(reads - center), axis=-1, keepdims=True))
    state_branch = (((reads - center) * lax.rsqrt(variance + group_eps)).reshape(STREAM_LENGTH, MIX_WIDTH) * head_gain).astype(jnp.bfloat16)
    total = jnp.dot(conv_branch, readout_projector[:MIX_WIDTH], preferred_element_type=jnp.float32) + jnp.dot(state_branch, readout_projector[MIX_WIDTH:], preferred_element_type=jnp.float32)
    return total.astype(jnp.bfloat16)
```

```python
import jax
import jax.numpy as jnp
from jax import lax
from jax.experimental import pallas as pl
from jax.experimental.pallas import tpu as pltpu
from jax.sharding import PartitionSpec as P

HEAD_SIZE = 64


norm_eps = 1e-05
group_eps = 0.00064
unit_eps = 1e-06
highest = lax.Precision.HIGHEST


def prefix_2(shard, axis, join, neutral):
    place = lax.axis_index(axis)
    gathered = jax.tree.map(
        lambda a, kind: lax.all_gather(a.astype(kind), axis),
        shard,
        jax.tree.map(lambda a: jnp.bfloat16 if a.dtype == jnp.float32 else a.dtype, shard),
    )
    state = jax.tree.map(lambda a, e: jnp.zeros_like(a) + jnp.asarray(e, a.dtype), shard, neutral)

    def one(hop, state):
        return join(
            state,
            jax.tree.map(
                lambda a, own: lax.dynamic_index_in_dim(a, hop, 0, False).astype(own.dtype),
                gathered,
                shard,
            ),
        )

    return lax.fori_loop(0, place, one, state)


def shifted(value, axis, steps):
    count = lax.axis_size(axis)
    first, last = (max(0, -steps), min(count, count - steps))
    return lax.ppermute(value, axis, [(source, source + steps) for source in range(first, last)])


def compose(earlier, later):
    return (
        jnp.einsum("hij,hjk->hik", earlier[0], later[0], precision=highest),
        jnp.einsum("hij,hjk->hik", earlier[1], later[0], precision=highest) + later[1],
    )


def state_mixer(recept, keys, values, decay_proj, decay_base, decay_shift, rate_logit, head_gain):
    rows, cols = recept.shape
    heads = cols // HEAD_SIZE
    span = min(64, rows // 2)
    blocks = rows // span
    pre = decay_base + decay_proj.astype(jnp.float32) + decay_shift
    log_decay = -jnp.exp(-jax.nn.softplus(-pre) - 0.5)
    rate = jax.nn.sigmoid(rate_logit).reshape(heads, HEAD_SIZE)

    def blocked(array):
        return array.astype(jnp.float32).reshape(blocks, span, heads, HEAD_SIZE)

    query_rows = blocked(recept)
    key_rows = blocked(keys)
    value_rows = blocked(values)
    decay_rows = blocked(log_decay)
    unit = key_rows * lax.rsqrt(jnp.sum(key_rows * key_rows, axis=-1, keepdims=True) + unit_eps)
    beta_rows = unit * rate
    running = jnp.cumsum(decay_rows, axis=1)
    before = running - decay_rows
    closing_position = running[:, -1:]
    query_dec = query_rows * jnp.exp(running)
    alpha_dec = -unit * jnp.exp(before)
    key_inv = key_rows * jnp.exp(-running)
    inverse_beta_matrix = beta_rows * jnp.exp(-running)
    key_end = key_rows * jnp.exp(closing_position - running)
    beta_end = beta_rows * jnp.exp(closing_position - running)
    order = jnp.arange(span)
    exclusive_triangle = order[:, None] > order[None, :]
    inclusive = order[:, None] >= order[None, :]

    def pairs(left, right, mask):
        inner = jnp.einsum("bthn,bshn->bhts", left, right, precision=highest)
        return jnp.where(mask, inner, 0.0)

    alpha_beta = pairs(alpha_dec, inverse_beta_matrix, exclusive_triangle)
    alpha_key = pairs(alpha_dec, key_inv, exclusive_triangle)
    query_beta = pairs(query_dec, inverse_beta_matrix, inclusive)
    query_key = pairs(query_dec, key_inv, inclusive)
    value_heads = jnp.swapaxes(value_rows, 1, 2)
    right_side = jnp.concatenate(
        [
            jnp.swapaxes(alpha_dec, 1, 2),
            jnp.einsum("bhts,bhsn->bhtn", alpha_key, value_heads, precision=highest),
        ],
        axis=-1,
    )
    eye_span = jnp.eye(span, dtype=jnp.float32)
    solved = jax.scipy.linalg.solve_triangular(eye_span - alpha_beta, right_side, lower=True)
    mixing = solved[..., :HEAD_SIZE]
    base_rows = solved[..., HEAD_SIZE:]
    eye_head = jnp.eye(HEAD_SIZE, dtype=jnp.float32)
    transfer = jnp.exp(closing_position[:, 0])[..., None] * eye_head + jnp.einsum(
        "bhtk,bthj->bhkj", mixing, beta_end, precision=highest
    )
    added = jnp.einsum("bhtv,bthk->bhvk", base_rows, beta_end, precision=highest) + jnp.einsum(
        "bthv,bthk->bhvk", value_rows, key_end, precision=highest
    )
    query_all = jnp.swapaxes(query_dec, 1, 2) + jnp.einsum(
        "bhts,bhsk->bhtk", query_beta, mixing, precision=highest
    )
    local_read = jnp.einsum(
        "bhts,bhsv->bhtv", query_beta, base_rows, precision=highest
    ) + jnp.einsum("bhts,bhsv->bhtv", query_key, value_heads, precision=highest)
    eye_heads = jnp.broadcast_to(eye_head, (heads, HEAD_SIZE, HEAD_SIZE))
    zero_heads = jnp.zeros((heads, HEAD_SIZE, HEAD_SIZE), jnp.float32)

    def advance(carry, block):
        return (compose(carry, block), carry)

    device_maps, block_maps = lax.scan(advance, (eye_heads, zero_heads), (transfer, added))
    prefix = prefix_2(device_maps, "sp", compose, (eye_heads, zero_heads))
    entering = prefix[1]
    starts = (
        jnp.einsum("hvk,bhkj->bhvj", entering, block_maps[0], precision=highest) + block_maps[1]
    )
    reads = jnp.einsum("bhtk,bhvk->bhtv", query_all, starts, precision=highest) + local_read
    center = jnp.mean(reads, axis=-1, keepdims=True)
    variance = jnp.mean(jnp.square(reads - center), axis=-1, keepdims=True)
    normalized_rows = jnp.swapaxes(
        (reads - center) * lax.rsqrt(variance + group_eps), 1, 2
    ).reshape(rows, cols)
    return (normalized_rows * head_gain).astype(jnp.bfloat16)


def gathered_weights_body(
    tokens_in,
    norm_gain,
    recept_weight,
    key_weight,
    value_weight,
    decay_weight,
    outer_weight,
    inner_weight,
    conv_weight,
    conv_taps,
    decay_base,
    decay_shift,
    rate_logit,
    head_gain,
    readout_projector,
):
    whole = lax.all_gather(tokens_in, "tp", axis=1, tiled=True)
    wide = whole.astype(jnp.float32)
    center = jnp.mean(wide, axis=-1, keepdims=True)
    variance = jnp.mean(jnp.square(wide - center), axis=-1, keepdims=True)
    normalized_rows = ((wide - center) * lax.rsqrt(variance + norm_eps) * norm_gain).astype(
        jnp.bfloat16
    )
    pieces = (
        lax.all_gather(recept_weight, "sp", axis=0, tiled=True),
        lax.all_gather(key_weight, "sp", axis=0, tiled=True),
        lax.all_gather(value_weight, "sp", axis=0, tiled=True),
        lax.all_gather(decay_weight, "sp", axis=0, tiled=True),
        lax.all_gather(outer_weight, "sp", axis=0, tiled=True),
        lax.all_gather(inner_weight, "sp", axis=0, tiled=True),
        lax.all_gather(conv_weight, "sp", axis=0, tiled=True),
    )
    sums = tuple(
        (jnp.dot(normalized_rows, piece, preferred_element_type=jnp.float32) for piece in pieces)
    )
    recept, keys, values, decay_proj, outer, inner, conv_in = tuple(
        (total.astype(jnp.bfloat16) for total in sums)
    )
    gated = (inner.astype(jnp.float32) * conv_in.astype(jnp.float32)).astype(jnp.bfloat16)
    rim = shifted(gated[-2:], "sp", 1)
    padded = jnp.concatenate([rim, gated], axis=0).astype(jnp.float32)
    taps = conv_taps.astype(jnp.float32)
    conv_sum = taps[0] * padded[:-2] + taps[1] * padded[1:-1] + taps[2] * padded[2:]
    conv_branch = (outer.astype(jnp.float32) * conv_sum).astype(jnp.bfloat16)
    state_branch = state_mixer(
        recept, keys, values, decay_proj, decay_base, decay_shift, rate_logit, head_gain
    )
    output_rows = lax.all_gather(readout_projector, "sp", axis=0, tiled=True)
    half = output_rows.shape[0] // 2
    pieces = (
        lax.all_gather(conv_branch, "tp", axis=1, tiled=True),
        lax.all_gather(state_branch, "tp", axis=1, tiled=True),
    )
    count = pieces[0].shape[1]
    convolved_token_rows = lax.slice_in_dim(output_rows, 0, count, axis=0)
    state_rows = lax.dynamic_slice_in_dim(output_rows, half, count, 0)
    mixed = jnp.dot(pieces[0], convolved_token_rows, preferred_element_type=jnp.float32) + jnp.dot(
        pieces[1], state_rows, preferred_element_type=jnp.float32
    )
    return mixed.astype(jnp.bfloat16)


CHUNK = 128
STEP_CHUNKS = 4


def split(a):
    high = a.astype(jnp.bfloat16)
    return high, (a - high.astype(jnp.float32)).astype(jnp.bfloat16)


def dot3(a, b, dims=((1,), (0,))):
    def one(x, y):
        return lax.dot_general(x, y, (dims, ((), ())), preferred_element_type=jnp.float32)

    (ah, al), (bh, bl) = split(a), split(b)
    return one(ah, bh) + (one(ah, bl) + one(al, bh))


def unit_lower_inverse(lower, same_block):
    size = lower[0].shape[0]
    eye = jnp.where(same_block(1), 1.0, 0.0)
    base = [jnp.where(same_block(8), a, 0.0) for a in lower]
    squares = [dot3(a, a) for a in base]
    inverse = [eye + a for a in base]
    inverse = [x + dot3(x, s) for x, s in zip(inverse, squares)]
    fourth = [dot3(s, s) for s in squares]
    inverse = [x + dot3(x, s) for x, s in zip(inverse, fourth)]
    width = 8
    while width < size:
        off = jnp.logical_and(same_block(2 * width), jnp.logical_not(same_block(width)))
        right = [dot3(jnp.where(off, a, 0.0), x) for a, x in zip(lower, inverse)]
        inverse = [x + dot3(x, r) for x, r in zip(inverse, right)]
        width *= 2
    return inverse


def mixer_kernel(x_ref, w_ref, shift_ref, vec_ref, out_ref, state_ref, rim_ref):
    @pl.when(pl.program_id(0) == 0)
    def _():
        state_ref[...] = jnp.zeros_like(state_ref)
        rim_ref[...] = jnp.zeros_like(rim_ref)

    n = HEAD_SIZE
    rows = out_ref.shape[0]
    count = rows // CHUNK
    total = 0.0
    for i in range(x_ref.shape[1]):
        tokens = x_ref[:, i].reshape(rows, x_ref.shape[3])
        total += jnp.dot(tokens, w_ref[i], preferred_element_type=jnp.float32)
    total = total.astype(jnp.bfloat16).astype(jnp.float32)
    recept, keys, values, decay_proj, outer, inner, conv_in = (
        total[:, i * n : (i + 1) * n] for i in range(7)
    )
    gated = (inner * conv_in).astype(jnp.bfloat16).astype(jnp.float32)
    padded = jnp.concatenate([rim_ref[...], gated], axis=0)
    rim_ref[...] = gated[rows - 8 :]
    conv_sum = (
        vec_ref[3:4] * padded[6 : 6 + rows]
        + vec_ref[4:5] * padded[7 : 7 + rows]
        + vec_ref[5:6] * gated
    )
    conv_branch = outer * conv_sum

    pre = vec_ref[0:1] + decay_proj + shift_ref[...]
    log_decay = -(0.6065306597126334 / (1.0 + jnp.exp(-pre)))
    rate = 1.0 / (1.0 + jnp.exp(-vec_ref[1:2]))
    unit = keys * lax.rsqrt(jnp.sum(keys * keys, axis=-1, keepdims=True) + unit_eps)
    beta = unit * rate
    row = lax.broadcasted_iota(jnp.int32, (CHUNK, CHUNK), 0)
    col = lax.broadcasted_iota(jnp.int32, (CHUNK, CHUNK), 1)
    inclusive = row >= col
    strict = row > col
    triangle = jnp.where(inclusive, 1.0, 0.0)

    def same_block(width):
        return row // width == col // width

    def cut(a):
        return [a[g * CHUNK : (g + 1) * CHUNK] for g in range(count)]

    chunks = []
    for q, k, v, u, b, d in zip(*map(cut, (recept, keys, values, unit, beta, log_decay))):
        running = jnp.dot(
            triangle, d, preferred_element_type=jnp.float32, precision=highest
        )
        before = running - d
        middle = running[CHUNK // 2 - 1 : CHUNK // 2]
        closing = running[CHUNK - 1 :]
        grow = jnp.exp(middle - running)
        tail = jnp.exp(closing - running)
        left = jnp.concatenate(
            [-u * jnp.exp(before - middle), q * jnp.exp(running - middle)], axis=0
        )
        right = jnp.concatenate([b * grow, k * grow], axis=0)
        ends = jnp.concatenate([b * tail, k * tail], axis=0)
        chunks.append(
            (left, right, ends, -u * jnp.exp(before), q * jnp.exp(running), v, jnp.exp(closing))
        )
    pairs = [dot3(c[0], c[1], ((1,), (1,))) for c in chunks]
    alpha_key = [jnp.where(strict, p[:CHUNK, CHUNK:], 0.0) for p in pairs]
    pulled = [dot3(a, c[5]) for a, c in zip(alpha_key, chunks)]
    inverse = unit_lower_inverse(
        [jnp.where(strict, p[:CHUNK, :CHUNK], 0.0) for p in pairs], same_block
    )
    solved = [
        dot3(t, jnp.concatenate([c[3], p], axis=1)) for t, c, p in zip(inverse, chunks, pulled)
    ]
    stacked = [
        jnp.concatenate(
            [s, jnp.concatenate([jnp.zeros_like(c[5]), c[5]], axis=1)], axis=0
        )
        for s, c in zip(solved, chunks)
    ]
    both = jnp.concatenate([inclusive, inclusive], axis=1)
    local = [dot3(jnp.where(both, p[CHUNK:], 0.0), m) for p, m in zip(pairs, stacked)]
    maps = [dot3(m, c[2], ((0,), (0,))) for m, c in zip(stacked, chunks)]
    state = state_ref[...]
    reads = []
    for c, loc, step in zip(chunks, local, maps):
        reads.append(dot3(c[4] + loc[:, :n], state, ((1,), (1,))) + loc[:, n:])
        state = state * c[6] + dot3(state, step[:n]) + step[n:]
    state_ref[...] = state
    read = jnp.concatenate(reads, axis=0)
    read = read - jnp.mean(read, axis=-1, keepdims=True)
    variance = jnp.mean(read * read, axis=-1, keepdims=True)
    state_branch = read * lax.rsqrt(variance + group_eps) * vec_ref[2:3]
    out_ref[...] = jnp.concatenate([conv_branch, state_branch], axis=1).astype(out_ref.dtype)


def run_mixer(normed, weights, shift, vectors):
    blocks, halves, own, depth = normed.shape
    width = weights.shape[-1]
    rows = STEP_CHUNKS * CHUNK
    length = blocks * own
    return pl.pallas_call(
        mixer_kernel,
        grid=(length // rows,),
        out_shape=jax.ShapeDtypeStruct((length, 2 * HEAD_SIZE), jnp.bfloat16),
        in_specs=[
            pl.BlockSpec((rows // own, halves, own, depth), lambda i: (i, 0, 0, 0)),
            pl.BlockSpec((halves, depth, width), lambda i: (0, 0, 0)),
            pl.BlockSpec((rows, HEAD_SIZE), lambda i: (i, 0)),
            pl.BlockSpec((8, HEAD_SIZE), lambda i: (0, 0)),
        ],
        out_specs=pl.BlockSpec((rows, 2 * HEAD_SIZE), lambda i: (i, 0)),
        scratch_shapes=[
            pltpu.VMEM((HEAD_SIZE, HEAD_SIZE), jnp.float32),
            pltpu.VMEM((8, HEAD_SIZE), jnp.float32),
        ],
        compiler_params=pltpu.CompilerParams(
            dimension_semantics=("arbitrary",), vmem_limit_bytes=40 * 1024 * 1024
        ),
        cost_estimate=pl.CostEstimate(
            flops=60_000_000_000, bytes_accessed=length * depth * 4, transcendentals=0
        ),
    )(normed, weights, shift, vectors)


def head_body(
    tokens_in,
    norm_gain,
    recept_weight,
    key_weight,
    value_weight,
    decay_weight,
    outer_weight,
    inner_weight,
    conv_weight,
    conv_taps,
    decay_base,
    decay_shift,
    rate_logit,
    head_gain,
    readout_projector,
):
    count = lax.axis_size("sp")
    halves = lax.axis_size("tp")
    place = lax.axis_index("sp")
    side = lax.axis_index("tp")
    rows, cols = tokens_in.shape

    wide = tokens_in.astype(jnp.float32)
    part_mean = jnp.mean(wide, axis=-1)
    part_square = jnp.sum(jnp.square(wide - part_mean[:, None]), axis=-1)
    parts = lax.all_gather(jnp.stack([part_mean, part_square]), "tp", axis=0)
    center = jnp.mean(parts[:, 0], axis=0)
    variance = (
        jnp.sum(parts[:, 1], axis=0) + cols * jnp.sum(jnp.square(parts[:, 0] - center), axis=0)
    ) / (cols * halves)
    gain = lax.dynamic_slice_in_dim(norm_gain, side * cols, cols, 0)
    normed = (
        (wide - center[:, None]) * lax.rsqrt(variance + norm_eps)[:, None] * gain
    ).astype(jnp.bfloat16)
    normed = lax.all_gather(normed, ("sp", "tp"), axis=0)
    normed, readout_projector = lax.optimization_barrier((normed, readout_projector))
    normed = normed.reshape(count, halves, rows, cols)

    weights = jnp.stack(
        [
            recept_weight,
            key_weight,
            value_weight,
            decay_weight,
            outer_weight,
            inner_weight,
            conv_weight,
        ]
    )
    kinds, depth = weights.shape[:2]
    weights = weights.reshape(kinds, depth, count, HEAD_SIZE).transpose(2, 1, 0, 3)
    weights = weights.reshape(count, depth, kinds * HEAD_SIZE)
    weights = lax.all_to_all(weights, "sp", 0, 0, tiled=True)
    weights = weights.reshape(halves, cols, kinds * HEAD_SIZE)
    shift = decay_shift.reshape(rows, count, HEAD_SIZE).transpose(1, 0, 2)
    shift = lax.all_to_all(shift, "sp", 0, 0, tiled=True).reshape(count * rows, HEAD_SIZE)
    vectors = jnp.concatenate(
        [
            jnp.stack([decay_base, rate_logit, head_gain]),
            conv_taps.astype(jnp.float32),
            jnp.zeros((2, cols), jnp.float32),
        ]
    )
    vectors = lax.dynamic_slice_in_dim(vectors, place * HEAD_SIZE, HEAD_SIZE, 1)
    branches = run_mixer(normed, weights, shift, vectors)
    branches = branches.reshape(count, rows, 2 * HEAD_SIZE)
    branches = lax.all_to_all(branches, "sp", 0, 0, tiled=True)
    branches = branches.reshape(count, rows, 2, HEAD_SIZE).transpose(1, 2, 0, 3)
    branches = branches.reshape(rows, 2 * cols)
    branches = lax.all_gather(branches, "tp", axis=0)
    output_rows = lax.all_gather(readout_projector, "sp", axis=0, tiled=True)
    output_rows = output_rows.reshape(2, halves, cols, cols)
    mixed = 0.0
    for i in range(halves):
        for branch in range(2):
            mixed += jnp.dot(
                branches[i, :, branch * cols : (branch + 1) * cols],
                output_rows[branch, i],
                preferred_element_type=jnp.float32,
            )
    return mixed.astype(jnp.bfloat16)


def body(*args):
    rows, cols = args[0].shape
    count = lax.axis_size("sp")
    if cols == count * HEAD_SIZE and STEP_CHUNKS * CHUNK % rows == 0:
        return head_body(*args)
    return gathered_weights_body(*args)


def solution(mesh):
    in_specs = (
        P("sp", "tp"),
        P(),
        P("sp", "tp"),
        P("sp", "tp"),
        P("sp", "tp"),
        P("sp", "tp"),
        P("sp", "tp"),
        P("sp", "tp"),
        P("sp", "tp"),
        P(None, "tp"),
        P("tp"),
        P("sp", "tp"),
        P("tp"),
        P("tp"),
        P("sp", "tp"),
    )
    out_specs = P("sp", "tp")
    return jax.shard_map(body, mesh=mesh, in_specs=in_specs, out_specs=out_specs, check_vma=False)
```

```python
import jax
import jax.numpy as jnp
from jax import lax
from jax.experimental import pallas as pl
from jax.experimental.pallas import tpu as pltpu
from jax.sharding import PartitionSpec as P

HEAD_SIZE = 64


norm_eps = 1e-05
group_eps = 0.00064
unit_eps = 1e-06
highest = lax.Precision.HIGHEST


def prefix_2(shard, axis, join, neutral):
    place = lax.axis_index(axis)
    gathered = jax.tree.map(
        lambda a, kind: lax.all_gather(a.astype(kind), axis),
        shard,
        jax.tree.map(lambda a: jnp.bfloat16 if a.dtype == jnp.float32 else a.dtype, shard),
    )
    state = jax.tree.map(lambda a, e: jnp.zeros_like(a) + jnp.asarray(e, a.dtype), shard, neutral)

    def one(hop, state):
        return join(
            state,
            jax.tree.map(
                lambda a, own: lax.dynamic_index_in_dim(a, hop, 0, False).astype(own.dtype),
                gathered,
                shard,
            ),
        )

    return lax.fori_loop(0, place, one, state)


def shifted(value, axis, steps):
    count = lax.axis_size(axis)
    first, last = (max(0, -steps), min(count, count - steps))
    return lax.ppermute(value, axis, [(source, source + steps) for source in range(first, last)])


def compose(earlier, later):
    return (
        jnp.einsum("hij,hjk->hik", earlier[0], later[0], precision=highest),
        jnp.einsum("hij,hjk->hik", earlier[1], later[0], precision=highest) + later[1],
    )


def state_mixer(recept, keys, values, decay_proj, decay_base, decay_shift, rate_logit, head_gain):
    rows, cols = recept.shape
    heads = cols // HEAD_SIZE
    span = min(64, rows // 2)
    blocks = rows // span
    pre = decay_base + decay_proj.astype(jnp.float32) + decay_shift
    log_decay = -jnp.exp(-jax.nn.softplus(-pre) - 0.5)
    rate = jax.nn.sigmoid(rate_logit).reshape(heads, HEAD_SIZE)

    def blocked(array):
        return array.astype(jnp.float32).reshape(blocks, span, heads, HEAD_SIZE)

    query_rows = blocked(recept)
    key_rows = blocked(keys)
    value_rows = blocked(values)
    decay_rows = blocked(log_decay)
    unit = key_rows * lax.rsqrt(jnp.sum(key_rows * key_rows, axis=-1, keepdims=True) + unit_eps)
    beta_rows = unit * rate
    running = jnp.cumsum(decay_rows, axis=1)
    before = running - decay_rows
    closing_position = running[:, -1:]
    query_dec = query_rows * jnp.exp(running)
    alpha_dec = -unit * jnp.exp(before)
    key_inv = key_rows * jnp.exp(-running)
    inverse_beta_matrix = beta_rows * jnp.exp(-running)
    key_end = key_rows * jnp.exp(closing_position - running)
    beta_end = beta_rows * jnp.exp(closing_position - running)
    order = jnp.arange(span)
    exclusive_triangle = order[:, None] > order[None, :]
    inclusive = order[:, None] >= order[None, :]

    def pairs(left, right, mask):
        inner = jnp.einsum("bthn,bshn->bhts", left, right, precision=highest)
        return jnp.where(mask, inner, 0.0)

    alpha_beta = pairs(alpha_dec, inverse_beta_matrix, exclusive_triangle)
    alpha_key = pairs(alpha_dec, key_inv, exclusive_triangle)
    query_beta = pairs(query_dec, inverse_beta_matrix, inclusive)
    query_key = pairs(query_dec, key_inv, inclusive)
    value_heads = jnp.swapaxes(value_rows, 1, 2)
    right_side = jnp.concatenate(
        [
            jnp.swapaxes(alpha_dec, 1, 2),
            jnp.einsum("bhts,bhsn->bhtn", alpha_key, value_heads, precision=highest),
        ],
        axis=-1,
    )
    eye_span = jnp.eye(span, dtype=jnp.float32)
    solved = jax.scipy.linalg.solve_triangular(eye_span - alpha_beta, right_side, lower=True)
    mixing = solved[..., :HEAD_SIZE]
    base_rows = solved[..., HEAD_SIZE:]
    eye_head = jnp.eye(HEAD_SIZE, dtype=jnp.float32)
    transfer = jnp.exp(closing_position[:, 0])[..., None] * eye_head + jnp.einsum(
        "bhtk,bthj->bhkj", mixing, beta_end, precision=highest
    )
    added = jnp.einsum("bhtv,bthk->bhvk", base_rows, beta_end, precision=highest) + jnp.einsum(
        "bthv,bthk->bhvk", value_rows, key_end, precision=highest
    )
    query_all = jnp.swapaxes(query_dec, 1, 2) + jnp.einsum(
        "bhts,bhsk->bhtk", query_beta, mixing, precision=highest
    )
    local_read = jnp.einsum(
        "bhts,bhsv->bhtv", query_beta, base_rows, precision=highest
    ) + jnp.einsum("bhts,bhsv->bhtv", query_key, value_heads, precision=highest)
    eye_heads = jnp.broadcast_to(eye_head, (heads, HEAD_SIZE, HEAD_SIZE))
    zero_heads = jnp.zeros((heads, HEAD_SIZE, HEAD_SIZE), jnp.float32)

    def advance(carry, block):
        return (compose(carry, block), carry)

    device_maps, block_maps = lax.scan(advance, (eye_heads, zero_heads), (transfer, added))
    prefix = prefix_2(device_maps, "sp", compose, (eye_heads, zero_heads))
    entering = prefix[1]
    starts = (
        jnp.einsum("hvk,bhkj->bhvj", entering, block_maps[0], precision=highest) + block_maps[1]
    )
    reads = jnp.einsum("bhtk,bhvk->bhtv", query_all, starts, precision=highest) + local_read
    center = jnp.mean(reads, axis=-1, keepdims=True)
    variance = jnp.mean(jnp.square(reads - center), axis=-1, keepdims=True)
    normalized_rows = jnp.swapaxes(
        (reads - center) * lax.rsqrt(variance + group_eps), 1, 2
    ).reshape(rows, cols)
    return (normalized_rows * head_gain).astype(jnp.bfloat16)


def gathered_weights_body(
    tokens_in,
    norm_gain,
    recept_weight,
    key_weight,
    value_weight,
    decay_weight,
    outer_weight,
    inner_weight,
    conv_weight,
    conv_taps,
    decay_base,
    decay_shift,
    rate_logit,
    head_gain,
    readout_projector,
):
    whole = lax.all_gather(tokens_in, "tp", axis=1, tiled=True)
    wide = whole.astype(jnp.float32)
    center = jnp.mean(wide, axis=-1, keepdims=True)
    variance = jnp.mean(jnp.square(wide - center), axis=-1, keepdims=True)
    normalized_rows = ((wide - center) * lax.rsqrt(variance + norm_eps) * norm_gain).astype(
        jnp.bfloat16
    )
    pieces = (
        lax.all_gather(recept_weight, "sp", axis=0, tiled=True),
        lax.all_gather(key_weight, "sp", axis=0, tiled=True),
        lax.all_gather(value_weight, "sp", axis=0, tiled=True),
        lax.all_gather(decay_weight, "sp", axis=0, tiled=True),
        lax.all_gather(outer_weight, "sp", axis=0, tiled=True),
        lax.all_gather(inner_weight, "sp", axis=0, tiled=True),
        lax.all_gather(conv_weight, "sp", axis=0, tiled=True),
    )
    sums = tuple(
        (jnp.dot(normalized_rows, piece, preferred_element_type=jnp.float32) for piece in pieces)
    )
    recept, keys, values, decay_proj, outer, inner, conv_in = tuple(
        (total.astype(jnp.bfloat16) for total in sums)
    )
    gated = (inner.astype(jnp.float32) * conv_in.astype(jnp.float32)).astype(jnp.bfloat16)
    rim = shifted(gated[-2:], "sp", 1)
    padded = jnp.concatenate([rim, gated], axis=0).astype(jnp.float32)
    taps = conv_taps.astype(jnp.float32)
    conv_sum = taps[0] * padded[:-2] + taps[1] * padded[1:-1] + taps[2] * padded[2:]
    conv_branch = (outer.astype(jnp.float32) * conv_sum).astype(jnp.bfloat16)
    state_branch = state_mixer(
        recept, keys, values, decay_proj, decay_base, decay_shift, rate_logit, head_gain
    )
    output_rows = lax.all_gather(readout_projector, "sp", axis=0, tiled=True)
    half = output_rows.shape[0] // 2
    pieces = (
        lax.all_gather(conv_branch, "tp", axis=1, tiled=True),
        lax.all_gather(state_branch, "tp", axis=1, tiled=True),
    )
    count = pieces[0].shape[1]
    convolved_token_rows = lax.slice_in_dim(output_rows, 0, count, axis=0)
    state_rows = lax.dynamic_slice_in_dim(output_rows, half, count, 0)
    mixed = jnp.dot(pieces[0], convolved_token_rows, preferred_element_type=jnp.float32) + jnp.dot(
        pieces[1], state_rows, preferred_element_type=jnp.float32
    )
    return mixed.astype(jnp.bfloat16)


CHUNK = 128
STEP_CHUNKS = 4


def split(a):
    high = a.astype(jnp.bfloat16)
    return high, (a - high.astype(jnp.float32)).astype(jnp.bfloat16)


def dot3(a, b, dims=((1,), (0,))):
    def one(x, y):
        return lax.dot_general(x, y, (dims, ((), ())), preferred_element_type=jnp.float32)

    (ah, al), (bh, bl) = split(a), split(b)
    return one(ah, bh) + (one(ah, bl) + one(al, bh))


def unit_lower_inverse(lower, same_block):
    size = lower[0].shape[0]
    eye = jnp.where(same_block(1), 1.0, 0.0)
    base = [jnp.where(same_block(8), a, 0.0) for a in lower]
    squares = [dot3(a, a) for a in base]
    inverse = [eye + a for a in base]
    inverse = [x + dot3(x, s) for x, s in zip(inverse, squares)]
    fourth = [dot3(s, s) for s in squares]
    inverse = [x + dot3(x, s) for x, s in zip(inverse, fourth)]
    width = 8
    while width < size:
        off = jnp.logical_and(same_block(2 * width), jnp.logical_not(same_block(width)))
        right = [dot3(jnp.where(off, a, 0.0), x) for a, x in zip(lower, inverse)]
        inverse = [x + dot3(x, r) for x, r in zip(inverse, right)]
        width *= 2
    return inverse


def mixer_kernel(x_ref, w_ref, shift_ref, vec_ref, out_ref, state_ref, rim_ref):
    @pl.when(pl.program_id(0) == 0)
    def _():
        state_ref[...] = jnp.zeros_like(state_ref)
        rim_ref[...] = jnp.zeros_like(rim_ref)

    n = HEAD_SIZE
    rows = out_ref.shape[0]
    count = rows // CHUNK
    total = 0.0
    for i in range(x_ref.shape[1]):
        tokens = x_ref[:, i].reshape(rows, x_ref.shape[3])
        total += jnp.dot(tokens, w_ref[i], preferred_element_type=jnp.float32)
    total = total.astype(jnp.bfloat16).astype(jnp.float32)
    recept, keys, values, decay_proj, outer, inner, conv_in = (
        total[:, i * n : (i + 1) * n] for i in range(7)
    )
    gated = (inner * conv_in).astype(jnp.bfloat16).astype(jnp.float32)
    padded = jnp.concatenate([rim_ref[...], gated], axis=0)
    rim_ref[...] = gated[rows - 8 :]
    conv_sum = (
        vec_ref[3:4] * padded[6 : 6 + rows]
        + vec_ref[4:5] * padded[7 : 7 + rows]
        + vec_ref[5:6] * gated
    )
    conv_branch = outer * conv_sum

    pre = vec_ref[0:1] + decay_proj + shift_ref[...]
    log_decay = -(0.6065306597126334 / (1.0 + jnp.exp(-pre)))
    rate = 1.0 / (1.0 + jnp.exp(-vec_ref[1:2]))
    unit = keys * lax.rsqrt(jnp.sum(keys * keys, axis=-1, keepdims=True) + unit_eps)
    beta = unit * rate
    row = lax.broadcasted_iota(jnp.int32, (CHUNK, CHUNK), 0)
    col = lax.broadcasted_iota(jnp.int32, (CHUNK, CHUNK), 1)
    inclusive = row >= col
    strict = row > col
    triangle = jnp.where(inclusive, 1.0, 0.0)

    def same_block(width):
        return row // width == col // width

    def cut(a):
        return [a[g * CHUNK : (g + 1) * CHUNK] for g in range(count)]

    chunks = []
    for q, k, v, u, b, d in zip(*map(cut, (recept, keys, values, unit, beta, log_decay))):
        running = jnp.dot(
            triangle, d, preferred_element_type=jnp.float32, precision=highest
        )
        before = running - d
        middle = running[CHUNK // 2 - 1 : CHUNK // 2]
        closing = running[CHUNK - 1 :]
        grow = jnp.exp(middle - running)
        tail = jnp.exp(closing - running)
        left = jnp.concatenate(
            [-u * jnp.exp(before - middle), q * jnp.exp(running - middle)], axis=0
        )
        right = jnp.concatenate([b * grow, k * grow], axis=0)
        ends = jnp.concatenate([b * tail, k * tail], axis=0)
        chunks.append(
            (left, right, ends, -u * jnp.exp(before), q * jnp.exp(running), v, jnp.exp(closing))
        )
    pairs = [dot3(c[0], c[1], ((1,), (1,))) for c in chunks]
    alpha_key = [jnp.where(strict, p[:CHUNK, CHUNK:], 0.0) for p in pairs]
    pulled = [dot3(a, c[5]) for a, c in zip(alpha_key, chunks)]
    inverse = unit_lower_inverse(
        [jnp.where(strict, p[:CHUNK, :CHUNK], 0.0) for p in pairs], same_block
    )
    solved = [
        dot3(t, jnp.concatenate([c[3], p], axis=1)) for t, c, p in zip(inverse, chunks, pulled)
    ]
    stacked = [
        jnp.concatenate(
            [s, jnp.concatenate([jnp.zeros_like(c[5]), c[5]], axis=1)], axis=0
        )
        for s, c in zip(solved, chunks)
    ]
    both = jnp.concatenate([inclusive, inclusive], axis=1)
    local = [dot3(jnp.where(both, p[CHUNK:], 0.0), m) for p, m in zip(pairs, stacked)]
    maps = [dot3(m, c[2], ((0,), (0,))) for m, c in zip(stacked, chunks)]
    state = state_ref[...]
    reads = []
    for c, loc, step in zip(chunks, local, maps):
        reads.append(dot3(c[4] + loc[:, :n], state, ((1,), (1,))) + loc[:, n:])
        state = state * c[6] + dot3(state, step[:n]) + step[n:]
    state_ref[...] = state
    read = jnp.concatenate(reads, axis=0)
    read = read - jnp.mean(read, axis=-1, keepdims=True)
    variance = jnp.mean(read * read, axis=-1, keepdims=True)
    state_branch = read * lax.rsqrt(variance + group_eps) * vec_ref[2:3]
    out_ref[...] = jnp.concatenate([conv_branch, state_branch], axis=1).astype(out_ref.dtype)


def run_mixer(normed, weights, shift, vectors):
    blocks, halves, own, depth = normed.shape
    width = weights.shape[-1]
    rows = STEP_CHUNKS * CHUNK
    length = blocks * own
    return pl.pallas_call(
        mixer_kernel,
        grid=(length // rows,),
        out_shape=jax.ShapeDtypeStruct((length, 2 * HEAD_SIZE), jnp.bfloat16),
        in_specs=[
            pl.BlockSpec((rows // own, halves, own, depth), lambda i: (i, 0, 0, 0)),
            pl.BlockSpec((halves, depth, width), lambda i: (0, 0, 0)),
            pl.BlockSpec((rows, HEAD_SIZE), lambda i: (i, 0)),
            pl.BlockSpec((8, HEAD_SIZE), lambda i: (0, 0)),
        ],
        out_specs=pl.BlockSpec((rows, 2 * HEAD_SIZE), lambda i: (i, 0)),
        scratch_shapes=[
            pltpu.VMEM((HEAD_SIZE, HEAD_SIZE), jnp.float32),
            pltpu.VMEM((8, HEAD_SIZE), jnp.float32),
        ],
        compiler_params=pltpu.CompilerParams(
            dimension_semantics=("arbitrary",), vmem_limit_bytes=40 * 1024 * 1024
        ),
        cost_estimate=pl.CostEstimate(
            flops=60_000_000_000, bytes_accessed=length * depth * 4, transcendentals=0
        ),
    )(normed, weights, shift, vectors)


def head_body(
    tokens_in,
    norm_gain,
    recept_weight,
    key_weight,
    value_weight,
    decay_weight,
    outer_weight,
    inner_weight,
    conv_weight,
    conv_taps,
    decay_base,
    decay_shift,
    rate_logit,
    head_gain,
    readout_projector,
):
    count = lax.axis_size("sp")
    halves = lax.axis_size("tp")
    place = lax.axis_index("sp")
    side = lax.axis_index("tp")
    rows, cols = tokens_in.shape

    wide = tokens_in.astype(jnp.float32)
    part_mean = jnp.mean(wide, axis=-1)
    part_square = jnp.sum(jnp.square(wide - part_mean[:, None]), axis=-1)
    parts = lax.all_gather(jnp.stack([part_mean, part_square]), "tp", axis=0)
    center = jnp.mean(parts[:, 0], axis=0)
    variance = (
        jnp.sum(parts[:, 1], axis=0) + cols * jnp.sum(jnp.square(parts[:, 0] - center), axis=0)
    ) / (cols * halves)
    gain = lax.dynamic_slice_in_dim(norm_gain, side * cols, cols, 0)
    normed = (
        (wide - center[:, None]) * lax.rsqrt(variance + norm_eps)[:, None] * gain
    ).astype(jnp.bfloat16)
    normed = lax.all_gather(normed, ("sp", "tp"), axis=0)
    normed, readout_projector = lax.optimization_barrier((normed, readout_projector))
    output_rows = lax.all_gather(readout_projector, "sp", axis=0, tiled=True)
    output_rows = output_rows.reshape(2, halves, cols, cols)
    normed = normed.reshape(count, halves, rows, cols)

    weights = jnp.stack(
        [
            recept_weight,
            key_weight,
            value_weight,
            decay_weight,
            outer_weight,
            inner_weight,
            conv_weight,
        ]
    )
    kinds, depth = weights.shape[:2]
    weights = weights.reshape(kinds, depth, count, HEAD_SIZE).transpose(2, 1, 0, 3)
    weights = weights.reshape(count, depth, kinds * HEAD_SIZE)
    weights = lax.all_to_all(weights, "sp", 0, 0, tiled=True)
    weights = weights.reshape(halves, cols, kinds * HEAD_SIZE)
    shift = decay_shift.reshape(rows, count, HEAD_SIZE).transpose(1, 0, 2)
    shift = lax.all_to_all(shift, "sp", 0, 0, tiled=True).reshape(count * rows, HEAD_SIZE)
    vectors = jnp.concatenate(
        [
            jnp.stack([decay_base, rate_logit, head_gain]),
            conv_taps.astype(jnp.float32),
            jnp.zeros((2, cols), jnp.float32),
        ]
    )
    vectors = lax.dynamic_slice_in_dim(vectors, place * HEAD_SIZE, HEAD_SIZE, 1)
    branches = run_mixer(normed, weights, shift, vectors)
    branches = branches.reshape(count, rows, 2 * HEAD_SIZE)
    branches = lax.all_to_all(branches, "sp", 0, 0, tiled=True)
    branches = branches.reshape(count, rows, 2, HEAD_SIZE).transpose(1, 2, 0, 3)
    branches = branches.reshape(rows, 2 * cols)
    mixed = 0.0
    for step in range(halves):
        if step:
            turn = [(source, (source + step) % halves) for source in range(halves)]
            held = lax.ppermute(branches, "tp", turn)
        else:
            held = branches
        owner = lax.rem(side + halves - step, halves)
        for branch in range(2):
            mixed += jnp.dot(
                held[:, branch * cols : (branch + 1) * cols],
                lax.dynamic_index_in_dim(output_rows[branch], owner, 0, False),
                preferred_element_type=jnp.float32,
            )
    return mixed.astype(jnp.bfloat16)


def body(*args):
    rows, cols = args[0].shape
    count = lax.axis_size("sp")
    if cols == count * HEAD_SIZE and STEP_CHUNKS * CHUNK % rows == 0:
        return head_body(*args)
    return gathered_weights_body(*args)


def solution(mesh):
    in_specs = (
        P("sp", "tp"),
        P(),
        P("sp", "tp"),
        P("sp", "tp"),
        P("sp", "tp"),
        P("sp", "tp"),
        P("sp", "tp"),
        P("sp", "tp"),
        P("sp", "tp"),
        P(None, "tp"),
        P("tp"),
        P("sp", "tp"),
        P("tp"),
        P("tp"),
        P("sp", "tp"),
    )
    out_specs = P("sp", "tp")
    return jax.shard_map(body, mesh=mesh, in_specs=in_specs, out_specs=out_specs, check_vma=False)
```

```python
import jax
import jax.numpy as jnp
from jax import lax
from jax.experimental import pallas as pl
from jax.experimental.pallas import tpu as pltpu
from jax.sharding import PartitionSpec as P

HEAD_SIZE = 64


norm_eps = 1e-05
group_eps = 0.00064
unit_eps = 1e-06
highest = lax.Precision.HIGHEST


def prefix_2(shard, axis, join, neutral):
    place = lax.axis_index(axis)
    gathered = jax.tree.map(
        lambda a, kind: lax.all_gather(a.astype(kind), axis),
        shard,
        jax.tree.map(lambda a: jnp.bfloat16 if a.dtype == jnp.float32 else a.dtype, shard),
    )
    state = jax.tree.map(lambda a, e: jnp.zeros_like(a) + jnp.asarray(e, a.dtype), shard, neutral)

    def one(hop, state):
        return join(
            state,
            jax.tree.map(
                lambda a, own: lax.dynamic_index_in_dim(a, hop, 0, False).astype(own.dtype),
                gathered,
                shard,
            ),
        )

    return lax.fori_loop(0, place, one, state)


def shifted(value, axis, steps):
    count = lax.axis_size(axis)
    first, last = (max(0, -steps), min(count, count - steps))
    return lax.ppermute(value, axis, [(source, source + steps) for source in range(first, last)])


def compose(earlier, later):
    return (
        jnp.einsum("hij,hjk->hik", earlier[0], later[0], precision=highest),
        jnp.einsum("hij,hjk->hik", earlier[1], later[0], precision=highest) + later[1],
    )


def state_mixer(recept, keys, values, decay_proj, decay_base, decay_shift, rate_logit, head_gain):
    rows, cols = recept.shape
    heads = cols // HEAD_SIZE
    span = min(64, rows // 2)
    blocks = rows // span
    pre = decay_base + decay_proj.astype(jnp.float32) + decay_shift
    log_decay = -jnp.exp(-jax.nn.softplus(-pre) - 0.5)
    rate = jax.nn.sigmoid(rate_logit).reshape(heads, HEAD_SIZE)

    def blocked(array):
        return array.astype(jnp.float32).reshape(blocks, span, heads, HEAD_SIZE)

    query_rows = blocked(recept)
    key_rows = blocked(keys)
    value_rows = blocked(values)
    decay_rows = blocked(log_decay)
    unit = key_rows * lax.rsqrt(jnp.sum(key_rows * key_rows, axis=-1, keepdims=True) + unit_eps)
    beta_rows = unit * rate
    running = jnp.cumsum(decay_rows, axis=1)
    before = running - decay_rows
    closing_position = running[:, -1:]
    query_dec = query_rows * jnp.exp(running)
    alpha_dec = -unit * jnp.exp(before)
    key_inv = key_rows * jnp.exp(-running)
    inverse_beta_matrix = beta_rows * jnp.exp(-running)
    key_end = key_rows * jnp.exp(closing_position - running)
    beta_end = beta_rows * jnp.exp(closing_position - running)
    order = jnp.arange(span)
    exclusive_triangle = order[:, None] > order[None, :]
    inclusive = order[:, None] >= order[None, :]

    def pairs(left, right, mask):
        inner = jnp.einsum("bthn,bshn->bhts", left, right, precision=highest)
        return jnp.where(mask, inner, 0.0)

    alpha_beta = pairs(alpha_dec, inverse_beta_matrix, exclusive_triangle)
    alpha_key = pairs(alpha_dec, key_inv, exclusive_triangle)
    query_beta = pairs(query_dec, inverse_beta_matrix, inclusive)
    query_key = pairs(query_dec, key_inv, inclusive)
    value_heads = jnp.swapaxes(value_rows, 1, 2)
    right_side = jnp.concatenate(
        [
            jnp.swapaxes(alpha_dec, 1, 2),
            jnp.einsum("bhts,bhsn->bhtn", alpha_key, value_heads, precision=highest),
        ],
        axis=-1,
    )
    eye_span = jnp.eye(span, dtype=jnp.float32)
    solved = jax.scipy.linalg.solve_triangular(eye_span - alpha_beta, right_side, lower=True)
    mixing = solved[..., :HEAD_SIZE]
    base_rows = solved[..., HEAD_SIZE:]
    eye_head = jnp.eye(HEAD_SIZE, dtype=jnp.float32)
    transfer = jnp.exp(closing_position[:, 0])[..., None] * eye_head + jnp.einsum(
        "bhtk,bthj->bhkj", mixing, beta_end, precision=highest
    )
    added = jnp.einsum("bhtv,bthk->bhvk", base_rows, beta_end, precision=highest) + jnp.einsum(
        "bthv,bthk->bhvk", value_rows, key_end, precision=highest
    )
    query_all = jnp.swapaxes(query_dec, 1, 2) + jnp.einsum(
        "bhts,bhsk->bhtk", query_beta, mixing, precision=highest
    )
    local_read = jnp.einsum(
        "bhts,bhsv->bhtv", query_beta, base_rows, precision=highest
    ) + jnp.einsum("bhts,bhsv->bhtv", query_key, value_heads, precision=highest)
    eye_heads = jnp.broadcast_to(eye_head, (heads, HEAD_SIZE, HEAD_SIZE))
    zero_heads = jnp.zeros((heads, HEAD_SIZE, HEAD_SIZE), jnp.float32)

    def advance(carry, block):
        return (compose(carry, block), carry)

    device_maps, block_maps = lax.scan(advance, (eye_heads, zero_heads), (transfer, added))
    prefix = prefix_2(device_maps, "sp", compose, (eye_heads, zero_heads))
    entering = prefix[1]
    starts = (
        jnp.einsum("hvk,bhkj->bhvj", entering, block_maps[0], precision=highest) + block_maps[1]
    )
    reads = jnp.einsum("bhtk,bhvk->bhtv", query_all, starts, precision=highest) + local_read
    center = jnp.mean(reads, axis=-1, keepdims=True)
    variance = jnp.mean(jnp.square(reads - center), axis=-1, keepdims=True)
    normalized_rows = jnp.swapaxes(
        (reads - center) * lax.rsqrt(variance + group_eps), 1, 2
    ).reshape(rows, cols)
    return (normalized_rows * head_gain).astype(jnp.bfloat16)


def gathered_weights_body(
    tokens_in,
    norm_gain,
    recept_weight,
    key_weight,
    value_weight,
    decay_weight,
    outer_weight,
    inner_weight,
    conv_weight,
    conv_taps,
    decay_base,
    decay_shift,
    rate_logit,
    head_gain,
    readout_projector,
):
    whole = lax.all_gather(tokens_in, "tp", axis=1, tiled=True)
    wide = whole.astype(jnp.float32)
    center = jnp.mean(wide, axis=-1, keepdims=True)
    variance = jnp.mean(jnp.square(wide - center), axis=-1, keepdims=True)
    normalized_rows = ((wide - center) * lax.rsqrt(variance + norm_eps) * norm_gain).astype(
        jnp.bfloat16
    )
    pieces = (
        lax.all_gather(recept_weight, "sp", axis=0, tiled=True),
        lax.all_gather(key_weight, "sp", axis=0, tiled=True),
        lax.all_gather(value_weight, "sp", axis=0, tiled=True),
        lax.all_gather(decay_weight, "sp", axis=0, tiled=True),
        lax.all_gather(outer_weight, "sp", axis=0, tiled=True),
        lax.all_gather(inner_weight, "sp", axis=0, tiled=True),
        lax.all_gather(conv_weight, "sp", axis=0, tiled=True),
    )
    sums = tuple(
        (jnp.dot(normalized_rows, piece, preferred_element_type=jnp.float32) for piece in pieces)
    )
    recept, keys, values, decay_proj, outer, inner, conv_in = tuple(
        (total.astype(jnp.bfloat16) for total in sums)
    )
    gated = (inner.astype(jnp.float32) * conv_in.astype(jnp.float32)).astype(jnp.bfloat16)
    rim = shifted(gated[-2:], "sp", 1)
    padded = jnp.concatenate([rim, gated], axis=0).astype(jnp.float32)
    taps = conv_taps.astype(jnp.float32)
    conv_sum = taps[0] * padded[:-2] + taps[1] * padded[1:-1] + taps[2] * padded[2:]
    conv_branch = (outer.astype(jnp.float32) * conv_sum).astype(jnp.bfloat16)
    state_branch = state_mixer(
        recept, keys, values, decay_proj, decay_base, decay_shift, rate_logit, head_gain
    )
    output_rows = lax.all_gather(readout_projector, "sp", axis=0, tiled=True)
    half = output_rows.shape[0] // 2
    pieces = (
        lax.all_gather(conv_branch, "tp", axis=1, tiled=True),
        lax.all_gather(state_branch, "tp", axis=1, tiled=True),
    )
    count = pieces[0].shape[1]
    convolved_token_rows = lax.slice_in_dim(output_rows, 0, count, axis=0)
    state_rows = lax.dynamic_slice_in_dim(output_rows, half, count, 0)
    mixed = jnp.dot(pieces[0], convolved_token_rows, preferred_element_type=jnp.float32) + jnp.dot(
        pieces[1], state_rows, preferred_element_type=jnp.float32
    )
    return mixed.astype(jnp.bfloat16)


CHUNK = 128
STEP_CHUNKS = 4


def split(a):
    high = a.astype(jnp.bfloat16)
    return high, (a - high.astype(jnp.float32)).astype(jnp.bfloat16)


def dot3(a, b, dims=((1,), (0,))):
    def one(x, y):
        return lax.dot_general(x, y, (dims, ((), ())), preferred_element_type=jnp.float32)

    (ah, al), (bh, bl) = split(a), split(b)
    return one(ah, bh) + (one(ah, bl) + one(al, bh))


def unit_lower_inverse(lower, same_block):
    size = lower[0].shape[0]
    eye = jnp.where(same_block(1), 1.0, 0.0)
    base = [jnp.where(same_block(8), a, 0.0) for a in lower]
    squares = [dot3(a, a) for a in base]
    inverse = [eye + a for a in base]
    inverse = [x + dot3(x, s) for x, s in zip(inverse, squares)]
    fourth = [dot3(s, s) for s in squares]
    inverse = [x + dot3(x, s) for x, s in zip(inverse, fourth)]
    width = 8
    while width < size:
        off = jnp.logical_and(same_block(2 * width), jnp.logical_not(same_block(width)))
        right = [dot3(jnp.where(off, a, 0.0), x) for a, x in zip(lower, inverse)]
        inverse = [x + dot3(x, r) for x, r in zip(inverse, right)]
        width *= 2
    return inverse


def mixer_kernel(x_ref, w_ref, shift_ref, vec_ref, out_ref, state_ref, rim_ref):
    @pl.when(pl.program_id(0) == 0)
    def _():
        state_ref[...] = jnp.zeros_like(state_ref)
        rim_ref[...] = jnp.zeros_like(rim_ref)

    n = HEAD_SIZE
    rows = out_ref.shape[0]
    count = rows // CHUNK
    total = 0.0
    for i in range(x_ref.shape[1]):
        tokens = x_ref[:, i].reshape(rows, x_ref.shape[3])
        total += jnp.dot(tokens, w_ref[i], preferred_element_type=jnp.float32)
    total = total.astype(jnp.bfloat16).astype(jnp.float32)
    recept, keys, values, decay_proj, outer, inner, conv_in = (
        total[:, i * n : (i + 1) * n] for i in range(7)
    )
    gated = (inner * conv_in).astype(jnp.bfloat16).astype(jnp.float32)
    padded = jnp.concatenate([rim_ref[...], gated], axis=0)
    rim_ref[...] = gated[rows - 8 :]
    conv_sum = (
        vec_ref[3:4] * padded[6 : 6 + rows]
        + vec_ref[4:5] * padded[7 : 7 + rows]
        + vec_ref[5:6] * gated
    )
    conv_branch = outer * conv_sum

    pre = vec_ref[0:1] + decay_proj + shift_ref[...]
    log_decay = -(0.6065306597126334 / (1.0 + jnp.exp(-pre)))
    rate = 1.0 / (1.0 + jnp.exp(-vec_ref[1:2]))
    unit = keys * lax.rsqrt(jnp.sum(keys * keys, axis=-1, keepdims=True) + unit_eps)
    beta = unit * rate
    row = lax.broadcasted_iota(jnp.int32, (CHUNK, CHUNK), 0)
    col = lax.broadcasted_iota(jnp.int32, (CHUNK, CHUNK), 1)
    inclusive = row >= col
    strict = row > col
    triangle = jnp.where(inclusive, 1.0, 0.0)

    def same_block(width):
        return row // width == col // width

    def cut(a):
        return [a[g * CHUNK : (g + 1) * CHUNK] for g in range(count)]

    chunks = []
    for q, k, v, u, b, d in zip(*map(cut, (recept, keys, values, unit, beta, log_decay))):
        running = jnp.dot(
            triangle, d, preferred_element_type=jnp.float32, precision=highest
        )
        before = running - d
        middle = running[CHUNK // 2 - 1 : CHUNK // 2]
        closing = running[CHUNK - 1 :]
        grow = jnp.exp(middle - running)
        tail = jnp.exp(closing - running)
        left = jnp.concatenate(
            [-u * jnp.exp(before - middle), q * jnp.exp(running - middle)], axis=0
        )
        right = jnp.concatenate([b * grow, k * grow], axis=0)
        ends = jnp.concatenate([b * tail, k * tail], axis=0)
        chunks.append(
            (left, right, ends, -u * jnp.exp(before), q * jnp.exp(running), v, jnp.exp(closing))
        )
    pairs = [dot3(c[0], c[1], ((1,), (1,))) for c in chunks]
    alpha_key = [jnp.where(strict, p[:CHUNK, CHUNK:], 0.0) for p in pairs]
    pulled = [dot3(a, c[5]) for a, c in zip(alpha_key, chunks)]
    inverse = unit_lower_inverse(
        [jnp.where(strict, p[:CHUNK, :CHUNK], 0.0) for p in pairs], same_block
    )
    solved = [
        dot3(t, jnp.concatenate([c[3], p], axis=1)) for t, c, p in zip(inverse, chunks, pulled)
    ]
    stacked = [
        jnp.concatenate(
            [s, jnp.concatenate([jnp.zeros_like(c[5]), c[5]], axis=1)], axis=0
        )
        for s, c in zip(solved, chunks)
    ]
    both = jnp.concatenate([inclusive, inclusive], axis=1)
    local = [dot3(jnp.where(both, p[CHUNK:], 0.0), m) for p, m in zip(pairs, stacked)]
    maps = [dot3(m, c[2], ((0,), (0,))) for m, c in zip(stacked, chunks)]
    state = state_ref[...]
    reads = []
    for c, loc, step in zip(chunks, local, maps):
        reads.append(dot3(c[4] + loc[:, :n], state, ((1,), (1,))) + loc[:, n:])
        state = state * c[6] + dot3(state, step[:n]) + step[n:]
    state_ref[...] = state
    read = jnp.concatenate(reads, axis=0)
    read = read - jnp.mean(read, axis=-1, keepdims=True)
    variance = jnp.mean(read * read, axis=-1, keepdims=True)
    state_branch = read * lax.rsqrt(variance + group_eps) * vec_ref[2:3]
    out_ref[...] = jnp.concatenate([conv_branch, state_branch], axis=1).astype(out_ref.dtype)


def run_mixer(normed, weights, shift, vectors):
    blocks, halves, own, depth = normed.shape
    width = weights.shape[-1]
    rows = STEP_CHUNKS * CHUNK
    length = blocks * own
    return pl.pallas_call(
        mixer_kernel,
        grid=(length // rows,),
        out_shape=jax.ShapeDtypeStruct((length, 2 * HEAD_SIZE), jnp.bfloat16),
        in_specs=[
            pl.BlockSpec((rows // own, halves, own, depth), lambda i: (i, 0, 0, 0)),
            pl.BlockSpec((halves, depth, width), lambda i: (0, 0, 0)),
            pl.BlockSpec((rows, HEAD_SIZE), lambda i: (i, 0)),
            pl.BlockSpec((8, HEAD_SIZE), lambda i: (0, 0)),
        ],
        out_specs=pl.BlockSpec((rows, 2 * HEAD_SIZE), lambda i: (i, 0)),
        scratch_shapes=[
            pltpu.VMEM((HEAD_SIZE, HEAD_SIZE), jnp.float32),
            pltpu.VMEM((8, HEAD_SIZE), jnp.float32),
        ],
        compiler_params=pltpu.CompilerParams(
            dimension_semantics=("arbitrary",), vmem_limit_bytes=40 * 1024 * 1024
        ),
        cost_estimate=pl.CostEstimate(
            flops=60_000_000_000, bytes_accessed=length * depth * 4, transcendentals=0
        ),
    )(normed, weights, shift, vectors)


def head_body(
    tokens_in,
    norm_gain,
    recept_weight,
    key_weight,
    value_weight,
    decay_weight,
    outer_weight,
    inner_weight,
    conv_weight,
    conv_taps,
    decay_base,
    decay_shift,
    rate_logit,
    head_gain,
    readout_projector,
):
    count = lax.axis_size("sp")
    halves = lax.axis_size("tp")
    place = lax.axis_index("sp")
    side = lax.axis_index("tp")
    rows, cols = tokens_in.shape

    wide = tokens_in.astype(jnp.float32)
    part_mean = jnp.mean(wide, axis=-1)
    part_square = jnp.sum(jnp.square(wide - part_mean[:, None]), axis=-1)
    parts = lax.all_gather(jnp.stack([part_mean, part_square]), "tp", axis=0)
    center = jnp.mean(parts[:, 0], axis=0)
    variance = (
        jnp.sum(parts[:, 1], axis=0) + cols * jnp.sum(jnp.square(parts[:, 0] - center), axis=0)
    ) / (cols * halves)
    gain = lax.dynamic_slice_in_dim(norm_gain, side * cols, cols, 0)
    normed = (
        (wide - center[:, None]) * lax.rsqrt(variance + norm_eps)[:, None] * gain
    ).astype(jnp.bfloat16)
    normed = lax.all_gather(normed, ("sp", "tp"), axis=0)

    weights = jnp.stack(
        [
            recept_weight,
            key_weight,
            value_weight,
            decay_weight,
            outer_weight,
            inner_weight,
            conv_weight,
        ]
    )
    kinds, depth = weights.shape[:2]
    weights = weights.reshape(kinds, depth, count, HEAD_SIZE).transpose(2, 1, 0, 3)
    weights = weights.reshape(count, depth, kinds * HEAD_SIZE)
    weights = lax.all_to_all(weights, "sp", 0, 0, tiled=True)
    shift = decay_shift.reshape(rows, count, HEAD_SIZE).transpose(1, 0, 2)
    shift = lax.all_to_all(shift, "sp", 0, 0, tiled=True)
    normed, weights, shift, readout_projector = lax.optimization_barrier(
        (normed, weights, shift, readout_projector)
    )
    output_rows = lax.all_gather(readout_projector, "sp", axis=0, tiled=True)
    output_rows = output_rows.reshape(2, halves, cols, cols)
    normed = normed.reshape(count, halves, rows, cols)
    weights = weights.reshape(halves, cols, kinds * HEAD_SIZE)
    shift = shift.reshape(count * rows, HEAD_SIZE)
    vectors = jnp.concatenate(
        [
            jnp.stack([decay_base, rate_logit, head_gain]),
            conv_taps.astype(jnp.float32),
            jnp.zeros((2, cols), jnp.float32),
        ]
    )
    vectors = lax.dynamic_slice_in_dim(vectors, place * HEAD_SIZE, HEAD_SIZE, 1)
    branches = run_mixer(normed, weights, shift, vectors)
    branches = branches.reshape(count, rows, 2 * HEAD_SIZE)
    branches = lax.all_to_all(branches, "sp", 0, 0, tiled=True)
    branches = branches.reshape(count, rows, 2, HEAD_SIZE).transpose(1, 2, 0, 3)
    branches = branches.reshape(rows, 2 * cols)
    mixed = 0.0
    for step in range(halves):
        if step:
            turn = [(source, (source + step) % halves) for source in range(halves)]
            held = lax.ppermute(branches, "tp", turn)
        else:
            held = branches
        owner = lax.rem(side + halves - step, halves)
        for branch in range(2):
            mixed += jnp.dot(
                held[:, branch * cols : (branch + 1) * cols],
                lax.dynamic_index_in_dim(output_rows[branch], owner, 0, False),
                preferred_element_type=jnp.float32,
            )
    return mixed.astype(jnp.bfloat16)


def body(*args):
    rows, cols = args[0].shape
    count = lax.axis_size("sp")
    if cols == count * HEAD_SIZE and STEP_CHUNKS * CHUNK % rows == 0:
        return head_body(*args)
    return gathered_weights_body(*args)


def solution(mesh):
    in_specs = (
        P("sp", "tp"),
        P(),
        P("sp", "tp"),
        P("sp", "tp"),
        P("sp", "tp"),
        P("sp", "tp"),
        P("sp", "tp"),
        P("sp", "tp"),
        P("sp", "tp"),
        P(None, "tp"),
        P("tp"),
        P("sp", "tp"),
        P("tp"),
        P("tp"),
        P("sp", "tp"),
    )
    out_specs = P("sp", "tp")
    return jax.shard_map(body, mesh=mesh, in_specs=in_specs, out_specs=out_specs, check_vma=False)
```
